512 devices in a mesh: sp: 32 (over z, core), tp: 16 (over y, x).
Axes of the slice: x: 4, y: 4, z: 16, core: 2. Of those that a mesh axis runs over, the one named last changes fastest.
Arguments:
- u_val: bfloat16 [8192, 2048], P('sp', 'tp'), may hold values from -6 to 6
- u_gate: bfloat16 [8192, 2048], P('sp', 'tp'), may hold values from -9 to 9
- conv_weight: float32 [31, 2048], P(None, 'tp')
- conv_bias: float32 [2048], P('tp'), may hold values from -3 to 3
- ln_gain: float32 [2048], P('tp'), may hold values from 0.1 to 1.9
- ln_bias: float32 [2048], P('tp'), may hold values from -3 to 3
- proj_weight: bfloat16 [2048, 4096], P(None, 'tp'), may hold values from -0.125 to 0.125
- resid: bfloat16 [8192, 4096], P('sp', 'tp')
- norm_gain: float32 [4096], P('tp'), may hold values from 0.1 to 1.9
- route_ids: int32 [8192, 2], P('sp'), may hold values from 0 to 31, all different within a row; in each aligned block of 256 rows (0 to 255, 256 to 511, ...) at most 32 rows name the same one
- route_wts: float32 [8192, 2], P('sp'), may hold values from 0.3 to 1.5
- expert_gate: bfloat16 [32, 4096, 1024], P('sp', None, 'tp'), may hold values from -0.09375 to 0.09375
- expert_up: bfloat16 [32, 4096, 1024], P('sp', None, 'tp'), may hold values from -0.09375 to 0.09375
- expert_down: bfloat16 [32, 1024, 4096], P('sp', None, 'tp'), may hold values from -0.1875 to 0.1875
- shared_gate: bfloat16 [4096, 1024], P(None, 'tp'), may hold values from -0.09375 to 0.09375
- shared_up: bfloat16 [4096, 1024], P(None, 'tp'), may hold values from -0.09375 to 0.09375
- shared_down: bfloat16 [1024, 4096], P(None, 'tp'), may hold values from -0.1875 to 0.1875
Outputs:
- mixed: bfloat16 [8192, 4096], P('sp', 'tp')
The draws below stay inside these ranges and needn't reach their ends.
Inputs may be any that keep to these rules, and one draw needn't show every extreme that they name: `route_ids`: each row names 2 different experts. In each aligned block of 256 rows (the rows of one index of sp) no expert is named by more than 32 rows, a bound that some expert reaches in some blocks.
All inputs are finite; a program needn't handle non-finite values.
Results may differ from the reference program's by a relative error of at most 0.012.
Values may be sent and summed in bfloat16 or wider, within the bound.
A program may use at most 64 MiB of HBM per device.

```python
import math
import jax
import jax.numpy as jnp
import numpy as np
from jax import lax

D = 4096
CONV = 2048
EXPERT_HIDDEN = 1024
SHARED_HIDDEN = 1024
KERNEL = 31
TOP = 2
TOK_DEV = 256
TOKENS = 8192
EXPERTS = 32
CAP = 32
N_SP = 32


def draw_conv_weight(key, part):
    ramp = 4.0 ** (jnp.arange(CONV, dtype=jnp.float32) / (CONV - 1))
    base = jax.random.normal(key, (KERNEL, CONV), jnp.float32)
    return base * ramp[None, :] * KERNEL ** (-0.5)


def draw_resid(key, part):
    ramp = 3.0 ** (jnp.arange(D, dtype=jnp.float32) / (D - 1))
    base = jax.random.normal(key, (TOKENS, D), jnp.float32)
    return (base * ramp[None, :]).astype(jnp.bfloat16)


def levels(stream_key, shape, split, low, largest):
    def one(dim, blocks):
        steps = jax.random.uniform(jax.random.fold_in(jax.random.fold_in(stream_key, 6), dim), (blocks,), jnp.float32, low / len(split), largest / len(split))
        return jnp.repeat(jnp.exp(steps), shape[dim] // blocks).reshape((-1,) + (1,) * (len(shape) - dim - 1))

    gain = one(*split[0])
    for cut in split[1:]:
        gain = gain * one(*cut)
    return gain


def deal_out(own_key, own, number, rows, count, top, bound, lean):
    order = jax.random.permutation(own_key, count)
    crowded, common = shares(count, rows * top, bound, lean, True), shares(count, rows * top, bound, lean, False)
    places = jnp.arange(count)

    def named(tallies, offset_by):
        used = int((tallies > 0).sum())
        fixed = max(1, used // 4)
        moved = fixed + (places - fixed + offset_by * (used - fixed)) % max(1, count - fixed)
        return jnp.zeros((count,), jnp.int32).at[order[jnp.where(places < fixed, places, moved)]].set(jnp.asarray(tallies, jnp.int32))

    tallies = jnp.where(number % 4 == 0, named(crowded, number // 4), named(common, number - number // 4 - 1))
    mixed = jax.random.permutation(jax.random.fold_in(own, 3), count)
    source_of, taker = mixed[0:count // 2 * 2:2], mixed[1:count // 2 * 2:2]
    room = jnp.minimum(tallies[source_of] - 1, bound - tallies[taker]) // 2
    room = jnp.where((source_of == order[0]) | (taker == order[0]) | (tallies[taker] == 0), 0, jnp.maximum(room, 0))
    moved = jax.random.randint(jax.random.fold_in(own, 4), (count // 2,), 0, 1 << 20) % (room + 1)
    tallies = tallies.at[source_of].add(-moved).at[taker].add(moved)
    members = jnp.searchsorted(jnp.cumsum(tallies), jnp.arange(rows * top), side="right").astype(jnp.int32)
    listing = members.reshape(top, rows).T
    listing = listing[jax.random.permutation(jax.random.fold_in(own, 1), rows)]
    offset_by = jax.random.randint(jax.random.fold_in(own, 2), (rows, 1), 0, top)
    return jnp.take_along_axis(listing, (jnp.arange(top)[None, :] + offset_by) % top, axis=1)


def shares(amount, total, reach, lean, full):
    portions = [(1 << 20) // math.isqrt(standing ** lean) + 1 for standing in range(1, amount + 1)]
    largest = reach if full else min(reach, max(-(-total // amount), total * portions[0] // sum(portions)))
    least = 1 if total - largest >= amount - 1 else 0
    holding, rest = [largest] + [least] * (amount - 1), total - largest - least * (amount - 1)
    while rest > 0:
        free = [i for i in range(1, amount) if holding[i] < largest] or [i for i in range(1, amount) if holding[i] < reach]
        whole, left = sum([portions[i] for i in free]), rest
        for i in free:
            more = min(reach - holding[i], max(1, left * portions[i] // whole), rest)
            holding[i] = holding[i] + more
            rest = rest - more
    return np.array(holding)


def normal_values(stream_key, shape, scale, reach, split=(), kind=jnp.bfloat16):
    drawn = jax.random.normal(stream_key, shape, jnp.float32) * scale
    if len(split) > 0:
        drawn = levels(stream_key, shape, split, -0.22, 0.18) * drawn
    return jnp.clip(drawn, min=-reach, max=reach).astype(kind)


def setup_inputs(seed: int = 0) -> dict:
    arg_keys = jax.random.split(jax.random.key(seed), 18)
    u_val = normal_values(arg_keys[0], (TOKENS, CONV), 1.0, 6.0, ((0, 32), (1, 16)))
    u_gate = normal_values(arg_keys[1], (TOKENS, CONV), 1.5, 9.0, ((0, 32), (1, 16)))
    conv_weight = draw_conv_weight(jax.random.fold_in(arg_keys[17], 71), 0)
    conv_bias = normal_values(arg_keys[3], (CONV,), 0.5, 3.0, ((0, 16),), jnp.float32)
    ln_gain = jnp.clip(1.0 + 0.18 * jax.random.normal(arg_keys[4], (CONV,), jnp.float32), 0.1, 1.9)
    ln_bias = normal_values(arg_keys[5], (CONV,), 0.5, 3.0, ((0, 16),), jnp.float32)
    proj_weight = normal_values(arg_keys[6], (CONV, D), CONV ** -0.5, 0.125, ((1, 16),))
    resid = draw_resid(jax.random.fold_in(arg_keys[17], 71), 0)
    norm_gain = jnp.clip(1.0 + 0.18 * jax.random.normal(arg_keys[8], (D,), jnp.float32), 0.1, 1.9)
    route_ids_keys = jax.random.split(jax.random.fold_in(arg_keys[9], 1), TOKENS // TOK_DEV)
    route_ids_turns = jax.random.permutation(jax.random.fold_in(arg_keys[9], 3), TOKENS // TOK_DEV)
    route_ids = jax.vmap(lambda own, number: deal_out(jax.random.fold_in(arg_keys[9], 2), own, number, TOK_DEV, EXPERTS, TOP, CAP, 2))(route_ids_keys, route_ids_turns).reshape((TOKENS, TOP))
    route_wts = jnp.clip(0.3 + 1.2 * jax.random.uniform(arg_keys[10], (TOKENS, TOP), jnp.float32) ** levels(arg_keys[10], (TOKENS, TOP), ((0, 32),), -0.2, 0.2), 0.3, 1.5)
    expert_gate = normal_values(arg_keys[11], (EXPERTS, D, EXPERT_HIDDEN), D ** -0.5, 0.09375, ((0, 32), (2, 16)))
    expert_up = normal_values(arg_keys[12], (EXPERTS, D, EXPERT_HIDDEN), D ** -0.5, 0.09375, ((0, 32), (2, 16)))
    expert_down = normal_values(arg_keys[13], (EXPERTS, EXPERT_HIDDEN, D), EXPERT_HIDDEN ** -0.5, 0.1875, ((0, 32), (2, 16)))
    shared_gate = normal_values(arg_keys[14], (D, SHARED_HIDDEN), D ** -0.5, 0.09375, ((1, 16),))
    shared_up = normal_values(arg_keys[15], (D, SHARED_HIDDEN), D ** -0.5, 0.09375, ((1, 16),))
    shared_down = normal_values(arg_keys[16], (SHARED_HIDDEN, D), SHARED_HIDDEN ** -0.5, 0.1875, ((1, 16),))
    return {"u_val": u_val, "u_gate": u_gate, "conv_weight": conv_weight, "conv_bias": conv_bias, "ln_gain": ln_gain, "ln_bias": ln_bias, "proj_weight": proj_weight, "resid": resid, "norm_gain": norm_gain, "route_ids": route_ids, "route_wts": route_wts, "expert_gate": expert_gate, "expert_up": expert_up, "expert_down": expert_down, "shared_gate": shared_gate, "shared_up": shared_up, "shared_down": shared_down}


norm_eps = 1e-06

def slot_table(block_ids, block_wts):
    pair_ids = block_ids.reshape(-1)
    pair_wts = block_wts.reshape(-1)
    onehot = (pair_ids[:, None] == jnp.arange(EXPERTS, dtype=jnp.int32)[None, :]).astype(jnp.int32)
    before = jnp.cumsum(onehot, axis=0) - onehot
    position = lax.optimization_barrier(jnp.sum(before * onehot, axis=1))
    pair_slot = pair_ids * CAP + position
    matches = (jnp.arange(EXPERTS * CAP, dtype=jnp.int32)[:, None] == pair_slot[None, :]).astype(jnp.int32)
    pair_tok = (jnp.arange(TOK_DEV * TOP, dtype=jnp.int32) // TOP).astype(jnp.int32)
    filled = lax.optimization_barrier(jnp.sum(matches, axis=1))
    slot_tok = lax.optimization_barrier(jnp.sum(matches * pair_tok[None, :], axis=1)) + (1 - filled) * TOK_DEV
    slot_wts = lax.optimization_barrier(jnp.sum(matches.astype(jnp.float32) * pair_wts[None, :], axis=1))
    return (slot_tok.astype(jnp.int32), slot_wts)

def reference(u_val, u_gate, conv_weight, conv_bias, ln_gain, ln_bias, proj_weight, resid, norm_gain, route_ids, route_wts, expert_gate, expert_up, expert_down, shared_gate, shared_up, shared_down):
    gated = (u_val.astype(jnp.float32) * jax.nn.sigmoid(u_gate.astype(jnp.float32))).astype(jnp.bfloat16)
    gated = lax.optimization_barrier(gated).astype(jnp.float32)
    padded = jnp.concatenate([jnp.zeros((KERNEL - 1, CONV), jnp.float32), gated], axis=0)
    conv_sum = jnp.zeros((TOKENS, CONV), jnp.float32) + conv_bias[None, :]
    for tap_index in range(KERNEL):
        conv_sum = conv_sum + conv_weight[tap_index][None, :] * padded[tap_index:tap_index + TOKENS]
    channel_mean = lax.optimization_barrier(jnp.mean(conv_sum, axis=1, keepdims=True))
    centered = conv_sum - channel_mean
    channel_var = lax.optimization_barrier(jnp.mean(centered * centered, axis=1, keepdims=True))
    conv_out = jax.nn.silu(centered * lax.rsqrt(channel_var + norm_eps) * ln_gain + ln_bias).astype(jnp.bfloat16)
    projected = jnp.dot(conv_out, proj_weight, preferred_element_type=jnp.float32)
    residual_mid = (resid.astype(jnp.float32) + projected).astype(jnp.bfloat16)
    residual_wide = residual_mid.astype(jnp.float32)
    mean_square = lax.optimization_barrier(jnp.mean(residual_wide * residual_wide, axis=1, keepdims=True))
    normed_rows = (residual_wide * lax.rsqrt(mean_square + norm_eps) * norm_gain).astype(jnp.bfloat16)
    shared_hidden = (jax.nn.silu(jnp.dot(normed_rows, shared_gate, preferred_element_type=jnp.float32)) * jnp.dot(normed_rows, shared_up, preferred_element_type=jnp.float32)).astype(jnp.bfloat16)
    shared_out = jnp.dot(shared_hidden, shared_down, preferred_element_type=jnp.float32)
    slot_tok, slot_wts = jax.vmap(slot_table)(route_ids.reshape(N_SP, TOK_DEV, TOP), route_wts.reshape(N_SP, TOK_DEV, TOP))
    offsets = (jnp.arange(N_SP, dtype=jnp.int32) * TOK_DEV)[:, None]
    global_tok = jnp.where(slot_tok < TOK_DEV, slot_tok + offsets, TOKENS).astype(jnp.int32)
    global_tok = global_tok.reshape(N_SP, EXPERTS, CAP).transpose(1, 0, 2).reshape(EXPERTS, N_SP * CAP)
    slot_wts = slot_wts.reshape(N_SP, EXPERTS, CAP).transpose(1, 0, 2).reshape(EXPERTS, N_SP * CAP)
    rows_ext = jnp.concatenate([normed_rows, jnp.zeros((1, D), jnp.bfloat16)], axis=0)

    def expert_step(total, inputs):
        gate_w, up_w, down_w, tok_ids, tok_wts = inputs
        slot_rows = jnp.take(rows_ext, tok_ids, axis=0)
        hidden = (jax.nn.silu(jnp.dot(slot_rows, gate_w, preferred_element_type=jnp.float32)) * jnp.dot(slot_rows, up_w, preferred_element_type=jnp.float32)).astype(jnp.bfloat16)
        expert_out = jnp.dot(hidden, down_w, preferred_element_type=jnp.float32).astype(jnp.bfloat16)
        weighted = expert_out.astype(jnp.float32) * tok_wts[:, None]
        return (total + jax.ops.segment_sum(weighted, tok_ids, num_segments=TOKENS + 1), None)
    routed, _ = lax.scan(expert_step, jnp.zeros((TOKENS + 1, D), jnp.float32), (expert_gate, expert_up, expert_down, global_tok, slot_wts))
    return (residual_wide + shared_out + routed[:TOKENS]).astype(jnp.bfloat16)
```

```python
import jax
import jax.numpy as jnp
from jax import lax
from jax.experimental import pallas as pl
from jax.experimental.pallas import tpu as pltpu
from jax.sharding import PartitionSpec as P

MESH = pl.DeviceIdType.MESH
F32 = jnp.float32
BF16 = jnp.bfloat16

SP, TP, SIDE = 32, 16, 4
ROWS, CH, FEAT = 256, 128, 256
CONV, D = 2048, 4096
TAPS = 31
CAP = 32
SLOTS = SP * CAP
EPS = 1e-6


class Copies:
    def __init__(self, send, recv):
        self.send, self.recv, self.used, self.open = send, recv, 0, []

    def __call__(self, src, dst, target):
        k = self.used
        self.used += 1
        copy = pltpu.make_async_remote_copy(
            src_ref=src,
            dst_ref=dst,
            send_sem=self.send.at[k],
            recv_sem=self.recv.at[k],
            device_id=target,
            device_id_type=MESH,
        )
        copy.start()
        self.open.append(copy)
        return copy

    def drain(self):
        for copy in self.open:
            copy.wait_send()
        self.open = []


def wrap(i):
    return lax.rem(i + SIDE, SIDE)


class RingHalf:
    def __init__(self, copies, buf, lo, rows, first, y, x):
        self.copies, self.buf, self.lo, self.rows = copies, buf, lo, rows
        self.c1, self.c2 = (x, y) if first == "x" else (y, x)
        self.first = first

    def index(self, c1, c2):
        return c2 * SIDE + c1 if self.first == "x" else c1 * SIDE + c2

    def send(self, d1, d2, part, axis, step):
        half = self.rows // 2
        lo, n = {0: (self.lo, self.rows), 1: (self.lo, half), 2: (self.lo + half, half)}[part]
        src = self.index(wrap(self.c1 + d1), wrap(self.c2 + d2))
        ref = self.buf.at[src, pl.ds(lo, n)]
        to = (
            self.index(wrap(self.c1 + step), self.c2)
            if axis == 1
            else self.index(self.c1, wrap(self.c2 + step))
        )
        return self.copies(ref, ref, {"tp": to})

    def arrived(self, copy):
        copy.wait_recv()

    def rounds(self):
        one, two = {}, {}
        one["r"] = self.send(0, 0, 0, 1, 1)
        one["l"] = self.send(0, 0, 0, 1, -1)
        two[0] = (self.send(0, 0, 0, 2, 1), self.send(0, 0, 0, 2, -1))
        yield
        one["r"].wait_recv()
        fr = self.send(-1, 0, 1, 1, 1)
        two[-1] = (self.send(-1, 0, 0, 2, 1), self.send(-1, 0, 0, 2, -1))
        one["l"].wait_recv()
        fl = self.send(1, 0, 2, 1, -1)
        two[1] = (self.send(1, 0, 0, 2, 1), self.send(1, 0, 0, 2, -1))
        last = {}
        last[0] = self.forward(two, 0)
        yield
        fr.wait_recv()
        fl.wait_recv()
        two[2] = (self.send(2, 0, 0, 2, 1), self.send(2, 0, 0, 2, -1))
        last[-1] = self.forward(two, -1)
        last[1] = self.forward(two, 1)
        yield
        last[2] = self.forward(two, 2)
        for d in (0, -1, 1):
            for copy in last[d]:
                copy.wait_recv()
        yield
        for copy in last[2]:
            copy.wait_recv()

    def forward(self, two, d):
        right, left = two[d]
        right.wait_recv()
        a = self.send(d, -1, 1, 2, 1)
        left.wait_recv()
        b = self.send(d, 1, 2, 2, -1)
        return a, b


def gather_plane(copies, buf, rows, y, x):
    halves = (
        RingHalf(copies, buf, 0, rows // 2, "x", y, x).rounds(),
        RingHalf(copies, buf, rows // 2, rows // 2, "y", y, x).rounds(),
    )
    for _ in range(5):
        for half in halves:
            next(half, None)
        yield


def run(steps):
    for _ in steps:
        pass


def to_peers(copies, src, dst, me):
    return [copies(src, dst, {"tp": lax.rem(me + k, TP)}) for k in range(1, TP)]


def lanes(columns):
    rows = columns[0].shape[0]
    lane = lax.broadcasted_iota(jnp.int32, (rows, 128), 1)
    both = jnp.zeros((rows, 128), F32)
    for k, column in enumerate(columns):
        both = jnp.where(lane == k, column, both)
    return both.T


def columns(rows):
    n = rows[0].shape[1]
    sub = lax.broadcasted_iota(jnp.int32, (128, n), 0)
    both = jnp.zeros((128, n), F32)
    for k, row in enumerate(rows):
        both = jnp.where(sub == k, row, both)
    return both.T


def silu(v):
    return v / (1.0 + jnp.exp(-v))


def dot(a, b):
    return jnp.dot(a, b, preferred_element_type=F32)


def dot_t(a, b):
    return lax.dot_general(a, b, (((1,), (1,)), ((), ())), preferred_element_type=F32)


def kernel(
    u_val, u_gate, conv_weight, conv_bias, ln_gain, ln_bias, proj, resid, norm_gain, ids, wts,
    e_gate, e_up, e_down, s_gate, s_up, s_down,
    out,
    v_val, v_gate, v_cw, v_cb, v_lg, v_lb, v_proj, v_resid, v_ng, v_ids, v_wts,
    egu, sgu, w_lo, w_hi, s_lo, s_hi,
    in_sem,
    pad, conv, halo_out, halo_in, stat_out, stat_in, co, rm, ssq_out, ssq_in, na,
    disp, comb_hi, comb_lo, sent, got, ra, hid, back_out, back,
    send_sem, recv_sem,
):
    s, t = lax.axis_index("sp"), lax.axis_index("tp")
    y, x = t // SIDE, lax.rem(t, SIDE)

    barrier = pltpu.get_barrier_semaphore()
    for k in range(1, TP):
        pl.semaphore_signal(barrier, inc=1, device_id={"tp": lax.rem(t + k, TP)}, device_id_type=MESH)
    for k in range(1, SP):
        pl.semaphore_signal(barrier, inc=1, device_id={"sp": lax.rem(s + k, SP)}, device_id_type=MESH)

    loads = {}
    pairs = [
        (u_val, v_val), (u_gate, v_gate), (conv_weight, v_cw), (conv_bias, v_cb), (ln_gain, v_lg),
        (ln_bias, v_lb), (ids, v_ids), (wts, v_wts), (resid, v_resid), (norm_gain, v_ng), (proj, v_proj),
        (s_gate, sgu.at[pl.ds(0, 64)]), (s_up, sgu.at[pl.ds(64, 64)]),
        (e_gate.at[0], egu.at[pl.ds(0, 64)]), (e_up.at[0], egu.at[pl.ds(64, 64)]),
    ]
    for k, (src, dst) in enumerate(pairs):
        copy = pltpu.make_async_copy(src, dst, in_sem.at[k])
        copy.start()
        loads[k] = copy
    downs = []
    for k in range(TP):
        for n, (src, dst, at) in enumerate(
            ((e_down.at[0], w_lo, 0), (e_down.at[0], w_hi, 64), (s_down, s_lo, 0), (s_down, s_hi, 64))
        ):
            copy = pltpu.make_async_copy(
                src.at[pl.ds(64 * k, 64)], dst.at[k, pl.ds(at, 64)], in_sem.at[15 + 4 * k + n]
            )
            copy.start()
            downs.append(copy)
    for k in range(TP):
        for ref, at in ((w_lo, 64), (w_hi, 0), (s_lo, 64), (s_hi, 0)):
            ref[k, pl.ds(at, 64), :] = jnp.zeros((64, FEAT), BF16)

    copies = Copies(send_sem, recv_sem)

    for k in (0, 1):
        loads[k].wait()
    gate = v_gate[...].astype(F32)
    gated = (v_val[...].astype(F32) / (1.0 + jnp.exp(-gate))).astype(BF16)
    pad[pl.ds(32, ROWS), :] = gated.astype(F32)
    halo_out[...] = gated[ROWS - 32 :]

    for k in (6, 7):
        loads[k].wait()
    id_rows = v_ids[...].astype(F32)
    id_row = jnp.concatenate([id_rows[0:1], id_rows[1:2]], axis=1)
    expert = lax.broadcasted_iota(jnp.int32, (SP, 2 * ROWS), 0).astype(F32)
    named = (expert == id_row).astype(F32)
    earlier = (
        lax.broadcasted_iota(jnp.int32, (2 * ROWS, 2 * ROWS), 0)
        < lax.broadcasted_iota(jnp.int32, (2 * ROWS, 2 * ROWS), 1)
    ).astype(F32).astype(BF16)
    place = jnp.sum(dot(named.astype(BF16), earlier) * named, axis=0, keepdims=True)
    slot = id_row * CAP + place
    slot_0, slot_1 = slot[:, :ROWS], slot[:, ROWS:]
    row = lax.broadcasted_iota(jnp.int32, (SLOTS, ROWS), 0).astype(F32)
    disp[...] = jnp.where((row == slot_0) | (row == slot_1), 1.0, 0.0).astype(BF16)
    cols = columns([slot_0, slot_1, v_wts[0:1, :], v_wts[1:2, :]])
    col = lax.broadcasted_iota(jnp.int32, (ROWS, SLOTS), 1).astype(F32)
    weight = jnp.where(col == cols[:, 0:1], cols[:, 2:3], 0.0) + jnp.where(
        col == cols[:, 1:2], cols[:, 3:4], 0.0
    )
    high = weight.astype(BF16)
    comb_hi[...] = high
    comb_lo[...] = (weight - high.astype(F32)).astype(BF16)

    pl.semaphore_wait(barrier, TP - 1 + SP - 1)

    halo = copies(halo_out, halo_in, {"sp": lax.rem(s + 1, SP)})
    for k in (2, 3, 4, 5):
        loads[k].wait()
    halo.wait_recv()
    pad[pl.ds(0, 32), :] = jnp.where(s == 0, 0.0, halo_in[...].astype(F32))
    for part in range(2):
        total = jnp.broadcast_to(v_cb[...].reshape(1, CH), (128, CH))
        for tap in range(TAPS):
            total = total + v_cw[tap : tap + 1, :] * pad[pl.ds(128 * part + 2 + tap, 128), :]
        conv[pl.ds(128 * part, 128), :] = total

    mine = conv[...]
    mean = jnp.sum(mine, axis=1, keepdims=True) * (1.0 / CH)
    off = mine - mean
    stat_out[...] = lanes([mean, jnp.sum(off * off, axis=1, keepdims=True)])[0:8]
    stats = to_peers(copies, stat_out, stat_in.at[t], t)
    stat_in[t] = stat_out[...]
    for copy in stats:
        copy.wait_recv()
    means = stat_in[:, 0, :]
    total_mean = jnp.sum(means, axis=0, keepdims=True) * (1.0 / TP)
    off = means - total_mean
    var = (
        jnp.sum(stat_in[:, 1, :], axis=0, keepdims=True) + CH * jnp.sum(off * off, axis=0, keepdims=True)
    ) * (1.0 / CONV)
    cols = columns([total_mean, lax.rsqrt(var + EPS)])
    normed = (mine - cols[:, 0:1]) * cols[:, 1:2]
    co[t] = silu(normed * v_lg[...].reshape(1, CH) + v_lb[...].reshape(1, CH)).astype(BF16)
    run(gather_plane(copies, co, ROWS, y, x))

    for k in (8, 9, 10):
        loads[k].wait()
    acc = v_resid[...].astype(F32)
    for k in range(TP // 2):
        acc = acc + dot(jnp.concatenate([co[2 * k], co[2 * k + 1]], axis=1), v_proj[pl.ds(256 * k, 256), :])
    mid = acc.astype(BF16)
    rm[...] = mid
    wide = mid.astype(F32)
    ssq_out[...] = lanes([jnp.sum(wide * wide, axis=1, keepdims=True)])[0:8]
    squares = to_peers(copies, ssq_out, ssq_in.at[t], t)
    ssq_in[t] = ssq_out[...]
    for copy in squares:
        copy.wait_recv()
    scale = lax.rsqrt(jnp.sum(ssq_in[:, 0, :], axis=0, keepdims=True) * (1.0 / D) + EPS)
    na[t] = (wide * columns([scale])[:, 0:1] * v_ng[...].reshape(1, FEAT)).astype(BF16)

    rows = dot(disp[...], na[t]).astype(BF16)
    sent[...] = rows.reshape(SP, CAP, FEAT)
    moves = []
    for k in range(1, SP):
        e = lax.rem(s + SP - k, SP)
        moves.append(copies(sent.at[e], got.at[k], {"sp": e}))
    got[0] = sent[s]
    run(gather_plane(copies, na, ROWS, y, x))
    for k in (11, 12, 13, 14):
        loads[k].wait()
    lane = lax.broadcasted_iota(jnp.int32, (128, 128), 1)
    acc = jnp.zeros((ROWS, 128), F32)
    for k in range(TP):
        acc = acc + dot_t(na[k], sgu[:, pl.ds(FEAT * k, FEAT)])
    h = silu(acc) * pltpu.roll(acc, 64, axis=1)
    hid[t, pl.ds(512, 128), :] = jnp.where(lane < 64, h[:128], pltpu.roll(h[128:], 64, axis=1)).astype(BF16)

    for copy in moves:
        copy.wait_recv()
    ra[t] = got[...].reshape(SLOTS, FEAT)
    run(gather_plane(copies, ra, SLOTS, y, x))
    for part in range(4):
        lo, hi = pl.ds(128 * part, 128), pl.ds(512 + 128 * part, 128)
        a = jnp.zeros((128, 128), F32)
        b = jnp.zeros((128, 128), F32)
        for k in range(TP):
            w = egu[:, pl.ds(FEAT * k, FEAT)]
            a = a + dot_t(ra[k, lo, :], w)
            b = b + dot_t(ra[k, hi, :], w)
        a = silu(a) * pltpu.roll(a, 64, axis=1)
        b = silu(b) * pltpu.roll(b, 64, axis=1)
        hid[t, lo, :] = jnp.where(lane < 64, a, pltpu.roll(b, 64, axis=1)).astype(BF16)
    run(gather_plane(copies, hid, 640, y, x))

    for copy in downs:
        copy.wait()
    for part in range(4):
        for ref, at in ((w_lo, 0), (w_hi, 16)):
            acc = jnp.zeros((128, FEAT), F32)
            for k in range(TP):
                acc = acc + dot(hid[k, pl.ds(128 * part, 128), :], ref[k])
            back_out[pl.ds(at + 4 * part, 4)] = acc.astype(BF16).reshape(4, CAP, FEAT)
    moves = []
    for k in range(1, SP):
        moves.append(copies(back_out.at[k], back.at[s], {"sp": lax.rem(s + k, SP)}))
    back[s] = back_out[0]
    acc = rm[...].astype(F32)
    for n, ref in enumerate((s_lo, s_hi)):
        part = jnp.zeros((128, FEAT), F32)
        for k in range(TP):
            part = part + dot(hid[k, pl.ds(512, 128), :], ref[k])
        if n == 0:
            first = part
    acc = acc + jnp.concatenate([first, part], axis=0)
    for copy in moves:
        copy.wait_recv()
    full = back[...].reshape(SLOTS, FEAT)
    acc = acc + dot(comb_hi[...], full) + dot(comb_lo[...], full)
    out[...] = acc.astype(BF16)
    copies.drain()


def shards(*args):
    args = list(args)
    for k in (9, 10, 14, 15):
        args[k] = args[k].T
    for k in (11, 12):
        args[k] = jnp.swapaxes(args[k], 1, 2)
    bf, f = (lambda *shape: pltpu.VMEM(shape, BF16)), (lambda *shape: pltpu.VMEM(shape, F32))
    n_copies = 1 + 15 + 40 + 15 + 31 + 40 + 40 + 40 + 31
    return pl.pallas_call(
        kernel,
        name="layer",
        out_shape=jax.ShapeDtypeStruct((ROWS, FEAT), BF16),
        in_specs=[pl.BlockSpec(memory_space=pltpu.HBM)] * 17,
        out_specs=pl.BlockSpec(memory_space=pltpu.VMEM),
        scratch_shapes=[
            bf(ROWS, CH), bf(ROWS, CH), f(TAPS, CH), f(CH), f(CH), f(CH), bf(CONV, FEAT), bf(ROWS, FEAT), f(FEAT),
            pltpu.VMEM((2, ROWS), jnp.int32), f(2, ROWS),
            bf(128, D), bf(128, D),
            bf(TP, 128, FEAT), bf(TP, 128, FEAT), bf(TP, 128, FEAT), bf(TP, 128, FEAT),
            pltpu.SemaphoreType.DMA((15 + 64,)),
            f(32 + ROWS, CH), f(ROWS, CH), bf(32, CH), bf(32, CH), f(8, ROWS), f(TP, 8, ROWS), bf(TP, ROWS, CH),
            bf(ROWS, FEAT), f(8, ROWS), f(TP, 8, ROWS), bf(TP, ROWS, FEAT),
            bf(SLOTS, ROWS), bf(ROWS, SLOTS), bf(ROWS, SLOTS),
            bf(SP, CAP, FEAT), bf(SP, CAP, FEAT), bf(TP, SLOTS, FEAT), bf(TP, 640, 128),
            bf(SP, CAP, FEAT), bf(SP, CAP, FEAT),
            pltpu.SemaphoreType.DMA((n_copies,)), pltpu.SemaphoreType.DMA((n_copies,)),
        ],
        compiler_params=pltpu.CompilerParams(
            collective_id=0, has_side_effects=True, vmem_limit_bytes=60 * 2**20
        ),
    )(*args)


def solution(mesh):
    in_specs = (
        P("sp", "tp"), P("sp", "tp"), P(None, "tp"), P("tp"), P("tp"), P("tp"), P(None, "tp"), P("sp", "tp"), P("tp"),
        P("sp", None), P("sp", None), P("sp", None, "tp"), P("sp", None, "tp"), P("sp", None, "tp"),
        P(None, "tp"), P(None, "tp"), P(None, "tp"),
    )
    return jax.shard_map(shards, mesh=mesh, in_specs=in_specs, out_specs=P("sp", "tp"), check_vma=False)
```

```python
import heapq

import jax
import jax.numpy as jnp
from jax import lax
from jax.experimental import pallas as pl
from jax.experimental.pallas import tpu as pltpu
from jax.sharding import PartitionSpec as P

MESH = pl.DeviceIdType.MESH
F32 = jnp.float32
BF16 = jnp.bfloat16

SP, TP, SIDE = 32, 16, 4
ROWS, CH, FEAT = 256, 128, 256
CONV, D = 2048, 4096
TAPS = 31
CAP = 32
SLOTS = SP * CAP
CHUNKS = 4
SENDS, RECVS = 9 + 3 * CHUNKS, 5 + 24 * 3 + CHUNKS * (1 + 3 + 1 + 24)
ORDER = (3, 4, 2, 5, 1, 6, 0, 7)
EPS = 1e-6


def arrived(ref, sem):
    pltpu.make_async_copy(ref, ref, sem).wait()


class Copies:
    def __init__(self, send, recv):
        self.send, self.recv, self.sends, self.recvs, self.open = send, recv, 0, 0, []

    def group(self, ref):
        sem = self.send.at[self.sends]
        self.sends += 1
        self.open.append((ref, sem))
        return sem

    def landing(self):
        self.recvs += 1
        return self.recv.at[self.recvs - 1]

    def __call__(self, src, dst, target, send, recv):
        pltpu.make_async_remote_copy(
            src_ref=src, dst_ref=dst, send_sem=send, recv_sem=recv, device_id=target, device_id_type=MESH
        ).start()

    def drain(self):
        for ref, sem in self.open:
            arrived(ref, sem)


def wrap(i):
    return lax.rem(i + SIDE, SIDE)


class RingHalf:
    def __init__(self, copies, out, buf, lo, rows, first, y, x):
        self.copies, self.out, self.buf, self.lo, self.rows = copies, out, buf, lo, rows
        self.c1, self.c2 = (x, y) if first == "x" else (y, x)
        self.first = first

    def index(self, c1, c2):
        return c2 * SIDE + c1 if self.first == "x" else c1 * SIDE + c2

    def send(self, d1, d2, part, axis, step, sem=None):
        half = self.rows // 2
        lo, n = {0: (self.lo, self.rows), 1: (self.lo, half), 2: (self.lo + half, half)}[part]
        src = self.index(wrap(self.c1 + d1), wrap(self.c2 + d2))
        ref = self.buf.at[src, pl.ds(lo, n)]
        to = (
            self.index(wrap(self.c1 + step), self.c2)
            if axis == 1
            else self.index(self.c1, wrap(self.c2 + step))
        )
        sem = self.copies.landing() if sem is None else sem
        self.copies(ref, ref, {"tp": to}, self.out, sem)
        return sem

    def block(self, sem):
        arrived(self.buf.at[0, pl.ds(0, self.rows)], sem)

    def both(self, d):
        return self.send(d, 0, 0, 2, 1), self.send(d, 0, 0, 2, -1)

    def rounds(self):
        right = self.send(0, 0, 0, 1, 1)
        left = self.send(0, 0, 0, 1, -1)
        two = {0: self.both(0)}
        yield
        self.block(right)
        far = self.send(-1, 0, 1, 1, 1)
        two[-1] = self.both(-1)
        self.block(left)
        self.send(1, 0, 2, 1, -1, far)
        two[1] = self.both(1)
        last = self.copies.landing()
        self.forward(two, 0, last)
        yield
        self.block(far)
        two[2] = self.both(2)
        self.forward(two, -1, last)
        self.forward(two, 1, last)
        yield
        self.forward(two, 2, last)
        yield
        arrived(self.buf.at[pl.ds(0, 2)], last)

    def forward(self, two, d, last):
        right, left = two[d]
        self.block(right)
        self.send(d, -1, 1, 2, 1, last)
        self.block(left)
        self.send(d, 1, 2, 2, -1, last)


def gather_plane(copies, buf, rows, y, x):
    out = copies.group(buf.at[pl.ds(0, TP - 1)])
    halves = (
        RingHalf(copies, out, buf, 0, rows // 2, "x", y, x).rounds(),
        RingHalf(copies, out, buf, rows // 2, rows // 2, "y", y, x).rounds(),
    )
    for _ in range(5):
        for half in halves:
            next(half, None)
        yield


def run(steps):
    for _ in steps:
        pass


def ready(loads):
    while loads:
        arrived(*loads.pop())


def interleave(tasks):
    queue = [(at, n, task) for n, (at, task) in enumerate(tasks)]
    heapq.heapify(queue)
    while queue:
        now, n, task = heapq.heappop(queue)
        later = next(task, None)
        if later is not None:
            heapq.heappush(queue, (now + later, n, task))


def to_peers(copies, src, dst, me):
    out, sem = copies.group(dst.at[pl.ds(0, TP - 1)]), copies.landing()
    for k in range(1, TP):
        copies(src, dst.at[me], {"tp": lax.rem(me + k, TP)}, out, sem)
    return sem


def lanes(columns):
    rows = columns[0].shape[0]
    lane = lax.broadcasted_iota(jnp.int32, (rows, 128), 1)
    both = jnp.zeros((rows, 128), F32)
    for k, column in enumerate(columns):
        both = jnp.where(lane == k, column, both)
    return both.T


def columns(rows):
    n = rows[0].shape[1]
    sub = lax.broadcasted_iota(jnp.int32, (128, n), 0)
    both = jnp.zeros((128, n), F32)
    for k, row in enumerate(rows):
        both = jnp.where(sub == k, row, both)
    return both.T


def silu(v):
    return v / (1.0 + jnp.exp(-v))


def dot(a, b):
    return jnp.dot(a, b, preferred_element_type=F32)


def dot_t(a, b):
    return lax.dot_general(a, b, (((1,), (1,)), ((), ())), preferred_element_type=F32)


class Phases:
    def __init__(self):
        self.scope = None

    def __call__(self, name):
        if self.scope is not None:
            self.scope.__exit__(None, None, None)
        self.scope = jax.named_scope(name) if name else None
        if name:
            self.scope.__enter__()


def kernel(
    u_val, u_gate, conv_weight, conv_bias, ln_gain, ln_bias, proj, resid, norm_gain, ids, wts,
    e_gate, e_up, e_down, s_gate, s_up, s_down,
    out,
    v_val, v_gate, v_cw, v_cb, v_lg, v_lb, v_proj, v_resid, v_ng, v_ids, v_wts,
    ewt, w2, sgu, w_lo, w_hi, s_lo, s_hi,
    in_sem,
    pad, conv, halo_out, halo_in, stat_out, stat_in, co, rm, ssq_out, ssq_in, na,
    disp, comb_hi, comb_lo, sent, ya, rs_out, rs_in, hid, shared_out, back_out, back,
    send_sem, recv_sem,
):
    s, t = lax.axis_index("sp"), lax.axis_index("tp")
    y, x = t // SIDE, lax.rem(t, SIDE)

    phase = Phases()
    phase("start")
    barrier = pltpu.get_barrier_semaphore()
    for k in range(1, TP):
        pl.semaphore_signal(barrier, inc=1, device_id={"tp": lax.rem(t + k, TP)}, device_id_type=MESH)
    for k in range(1, SP):
        pl.semaphore_signal(barrier, inc=1, device_id={"sp": lax.rem(s + k, SP)}, device_id_type=MESH)

    loads = {}
    pairs = [
        (u_val, v_val), (u_gate, v_gate), (conv_weight, v_cw), (conv_bias, v_cb), (ln_gain, v_lg),
        (ln_bias, v_lb), (ids, v_ids), (wts, v_wts), (resid, v_resid), (norm_gain, v_ng), (proj, v_proj),
        (s_gate, sgu.at[pl.ds(0, 64)]), (s_up, sgu.at[pl.ds(64, 64)]),
    ]
    for k, (src, dst) in enumerate(pairs):
        copy = pltpu.make_async_copy(src, dst, in_sem.at[k])
        copy.start()
        loads[k] = copy
    for k in range(TP):
        for n, (src, dst, at) in enumerate(
            ((e_down.at[0], w_lo, 0), (e_down.at[0], w_hi, 64), (s_down, s_lo, 0), (s_down, s_hi, 64))
        ):
            pltpu.make_async_copy(
                src.at[pl.ds(64 * k, 64)], dst.at[k, pl.ds(at, 64)], in_sem.at[13 + n]
            ).start()
    downs = [(ref.at[pl.ds(0, TP // 2)], in_sem.at[13 + n]) for n, ref in enumerate((w_lo, w_hi, s_lo, s_hi))]
    for k in range(TP):
        for n, src in enumerate((e_gate, e_up)):
            pltpu.make_async_copy(
                src.at[0, :, pl.ds(FEAT * k, FEAT)], ewt.at[k, pl.ds(64 * n, 64)], in_sem.at[17]
            ).start()
    for k in range(TP):
        for ref, at in ((w_lo, 64), (w_hi, 0), (s_lo, 64), (s_hi, 0)):
            ref[k, pl.ds(at, 64), :] = jnp.zeros((64, FEAT), BF16)

    copies = Copies(send_sem, recv_sem)

    spread_out, spread_in = copies.group(w2.at[pl.ds(0, 3)]), copies.landing()

    def spread(k):
        for n in (2, 1, 3):
            to = wrap(x + n)
            copies(ewt.at[SIDE * k + to], w2.at[k, x], {"tp": y * SIDE + to}, spread_out, spread_in)

    phase("gated")
    for k in (0, 1):
        loads[k].wait()
    gate = v_gate[...].astype(F32)
    gated = (v_val[...].astype(F32) / (1.0 + jnp.exp(-gate))).astype(BF16)
    pad[pl.ds(32, ROWS), :] = gated.astype(F32)
    halo_out[...] = gated[ROWS - 32 :]

    phase("slots")
    for k in (6, 7):
        loads[k].wait()
    id_rows = v_ids[...].astype(F32)
    id_row = jnp.concatenate([id_rows[0:1], id_rows[1:2]], axis=1)
    expert = lax.broadcasted_iota(jnp.int32, (SP, 2 * ROWS), 0).astype(F32)
    named = (expert == id_row).astype(F32)
    earlier = (
        lax.broadcasted_iota(jnp.int32, (2 * ROWS, 2 * ROWS), 0)
        < lax.broadcasted_iota(jnp.int32, (2 * ROWS, 2 * ROWS), 1)
    ).astype(F32).astype(BF16)
    place = jnp.sum(dot(named.astype(BF16), earlier) * named, axis=0, keepdims=True)
    slot = id_row * CAP + place
    slot_0, slot_1 = slot[:, :ROWS], slot[:, ROWS:]
    row = lax.broadcasted_iota(jnp.int32, (SLOTS, ROWS), 0).astype(F32)
    disp[...] = jnp.where((row == slot_0) | (row == slot_1), 1.0, 0.0).astype(BF16)
    cols = columns([slot_0, slot_1, v_wts[0:1, :], v_wts[1:2, :]])
    col = lax.broadcasted_iota(jnp.int32, (ROWS, SLOTS), 1).astype(F32)
    weight = jnp.where(col == cols[:, 0:1], cols[:, 2:3], 0.0) + jnp.where(
        col == cols[:, 1:2], cols[:, 3:4], 0.0
    )
    high = weight.astype(BF16)
    comb_hi[...] = high
    comb_lo[...] = (weight - high.astype(F32)).astype(BF16)

    phase("barrier")
    pl.semaphore_wait(barrier, TP - 1 + SP - 1)

    phase("halo")
    halo = copies.landing()
    copies(halo_out, halo_in, {"sp": lax.rem(s + 1, SP)}, copies.group(halo_in), halo)
    for k in (2, 3, 4, 5):
        loads[k].wait()
    arrived(halo_in, halo)
    pad[pl.ds(0, 32), :] = jnp.where(s == 0, 0.0, halo_in[...].astype(F32))
    phase("conv")
    for part in range(2):
        total = jnp.broadcast_to(v_cb[...].reshape(1, CH), (128, CH))
        for tap in range(TAPS):
            total = total + v_cw[tap : tap + 1, :] * pad[pl.ds(128 * part + 2 + tap, 128), :]
        conv[pl.ds(128 * part, 128), :] = total

    phase("stats")
    mine = conv[...]
    mean = jnp.sum(mine, axis=1, keepdims=True) * (1.0 / CH)
    off = mine - mean
    stat_out[...] = lanes([mean, jnp.sum(off * off, axis=1, keepdims=True)])[0:8]
    stats = to_peers(copies, stat_out, stat_in, t)
    arrived(ewt, in_sem.at[17])
    spread(0)
    for k in range(SIDE):
        w2[k, x] = ewt[SIDE * k + x]
    stat_in[t] = stat_out[...]
    arrived(stat_in.at[pl.ds(0, TP - 1)], stats)
    means = stat_in[:, 0, :]
    total_mean = jnp.sum(means, axis=0, keepdims=True) * (1.0 / TP)
    off = means - total_mean
    var = (
        jnp.sum(stat_in[:, 1, :], axis=0, keepdims=True) + CH * jnp.sum(off * off, axis=0, keepdims=True)
    ) * (1.0 / CONV)
    cols = columns([total_mean, lax.rsqrt(var + EPS)])
    normed = (mine - cols[:, 0:1]) * cols[:, 1:2]
    co[t] = silu(normed * v_lg[...].reshape(1, CH) + v_lb[...].reshape(1, CH)).astype(BF16)
    phase("gather_co")
    run(gather_plane(copies, co, ROWS, y, x))

    phase("project")
    for k in (8, 9, 10):
        loads[k].wait()
    acc = v_resid[...].astype(F32)
    for k in range(TP // 2):
        acc = acc + dot(jnp.concatenate([co[2 * k], co[2 * k + 1]], axis=1), v_proj[pl.ds(256 * k, 256), :])
    mid = acc.astype(BF16)
    rm[...] = mid
    wide = mid.astype(F32)
    ssq_out[...] = lanes([jnp.sum(wide * wide, axis=1, keepdims=True)])[0:8]
    phase("ssq")
    squares = to_peers(copies, ssq_out, ssq_in, t)
    spread(1)
    ssq_in[t] = ssq_out[...]
    arrived(ssq_in.at[pl.ds(0, TP - 1)], squares)
    scale = lax.rsqrt(jnp.sum(ssq_in[:, 0, :], axis=0, keepdims=True) * (1.0 / D) + EPS)
    na[t] = (wide * columns([scale])[:, 0:1] * v_ng[...].reshape(1, FEAT)).astype(BF16)

    phase("dispatch")
    rows = dot(disp[...], na[t]).astype(BF16)
    sent[...] = rows.reshape(SP, CAP, FEAT)
    moves_out = copies.group(sent.at[pl.ds(0, SP - 1)])
    moves = [copies.landing() for c in range(CHUNKS)]

    def dispatch(c):
        phase(f"send{c}")
        for j in ORDER:
            k = CHUNKS * j + c
            if k:
                e = lax.rem(s + SP - k, SP)
                copies(sent.at[e], ya.at[c, y, pl.ds(CAP * j, CAP)], {"sp": e}, moves_out, moves[c])
        yield None

    ya[0, y, pl.ds(0, CAP), :] = sent[s]
    lane = lax.broadcasted_iota(jnp.int32, (128, 128), 1)

    def hidden(acc):
        h = silu(acc) * pltpu.roll(acc, 64, axis=1)
        return jnp.where(lane < 64, h[:128], pltpu.roll(h[128:], 64, axis=1)).astype(BF16)

    def down(c, lo, hi):
        both = []
        for ref in (lo, hi):
            acc = jnp.zeros((128, FEAT), F32)
            for k in range(TP // 2):
                pair = jnp.concatenate([hid[c, 2 * k], hid[c, 2 * k + 1]], axis=1)
                acc = acc + dot(pair, ref[pl.ds(2 * k, 2)].reshape(2 * 128, FEAT))
            both.append(acc)
        return both

    def more():
        for k in range(2, 4):
            spread(k)
        yield None

    def shared():
        phase("shared")
        for _ in gather_plane(copies, na, ROWS, y, x):
            yield 3.0
        for k in (11, 12):
            loads[k].wait()
        acc = jnp.zeros((ROWS, 128), F32)
        for k in range(TP):
            acc = acc + dot_t(na[k], sgu[:, pl.ds(FEAT * k, FEAT)])
        hid[CHUNKS, t] = hidden(acc)
        for _ in gather_plane(copies, hid.at[CHUNKS], 128, y, x):
            yield 4.0
        ready(downs)
        lo, hi = down(CHUNKS, s_lo, s_hi)
        shared_out[pl.ds(0, 128), :] = lo
        shared_out[pl.ds(128, 128), :] = hi

    returns_out, returns = copies.group(back.at[pl.ds(0, SP - 1)]), copies.landing()

    def routed(c):
        phase(f"arrive{c}")
        arrived(ya.at[c, 0, pl.ds(0 if c else CAP, ROWS if c else ROWS - CAP)], moves[c])
        out = copies.group(ya.at[c, pl.ds(0, 3)])
        a, b, far = copies.landing(), copies.landing(), copies.landing()
        up_y, down_y = {"tp": wrap(y + 1) * SIDE + x}, {"tp": wrap(y - 1) * SIDE + x}
        copies(ya.at[c, y], ya.at[c, y], up_y, out, a)
        copies(ya.at[c, y], ya.at[c, y], down_y, out, b)
        yield 4.5
        phase(f"ya{c}")
        arrived(ya.at[c, 0], a)
        at = ya.at[c, wrap(y - 1), pl.ds(0, 128)]
        copies(at, at, up_y, out, far)
        arrived(ya.at[c, 0], b)
        at = ya.at[c, wrap(y + 1), pl.ds(128, 128)]
        copies(at, at, down_y, out, far)
        yield 3.0
        phase(f"yb{c}")
        arrived(ya.at[c, 0], far)
        if c == 0:
            arrived(w2.at[pl.ds(0, 3)], spread_in)
        phase(f"up{c}")
        acc = jnp.zeros((ROWS, 4 * 128), F32)
        for k in range(SIDE):
            acc = acc + dot_t(ya[c, k], w2[k].reshape(4 * 128, FEAT))
        for k in range(SIDE):
            rs_out[c, k] = acc[:, 128 * k : 128 * (k + 1)].astype(BF16)
        out, parts = copies.group(rs_in.at[c, pl.ds(0, 3)]), copies.landing()
        for k in (2, 1, 3):
            to = wrap(x + k)
            copies(rs_out.at[c, to], rs_in.at[c, x], {"tp": y * SIDE + to}, out, parts)
        yield 5.0
        phase(f"rs{c}")
        arrived(rs_in.at[c, pl.ds(0, 3)], parts)
        acc = rs_out[c, x].astype(F32)
        for k in range(1, SIDE):
            acc = acc + rs_in[c, wrap(x + k)].astype(F32)
        hid[c, t] = hidden(acc)
        for n, _ in enumerate(gather_plane(copies, hid.at[c], 128, y, x)):
            yield 2.6
            phase(f"hid{c}{n}")
        ready(downs)
        phase(f"down{c}")
        lo, hi = down(c, w_lo, w_hi)
        back_out[c, pl.ds(0, 4)] = lo.astype(BF16).reshape(4, CAP, FEAT)
        back_out[c, pl.ds(4, 4)] = hi.astype(BF16).reshape(4, CAP, FEAT)
        for j in ORDER:
            k = CHUNKS * j + c
            if k:
                copies(back_out.at[c, j], back.at[s], {"sp": lax.rem(s + k, SP)}, returns_out, returns)

    tasks = [(4.5 * c, dispatch(c)) for c in range(CHUNKS)]
    tasks += [(0.0, more()), (0.1, shared())]
    tasks += [(10.0 + 4.5 * c, routed(c)) for c in range(CHUNKS)]
    interleave(tasks)
    back[s] = back_out[0, 0]
    phase("back_wait")
    arrived(back.at[pl.ds(0, SP - 1)], returns)
    phase("combine")
    full = back[...].reshape(SLOTS, FEAT)
    acc = rm[...].astype(F32) + shared_out[...] + dot(comb_hi[...], full) + dot(comb_lo[...], full)
    out[...] = acc.astype(BF16)
    phase("drain")
    copies.drain()
    assert (copies.sends, copies.recvs) == (SENDS, RECVS), (copies.sends, copies.recvs)
    phase(None)


def shards(*args):
    args = list(args)
    for k in (9, 10, 14, 15):
        args[k] = args[k].T
    for k in (11, 12):
        args[k] = jnp.swapaxes(args[k], 1, 2)
    bf, f = (lambda *shape: pltpu.VMEM(shape, BF16)), (lambda *shape: pltpu.VMEM(shape, F32))
    return pl.pallas_call(
        kernel,
        name="layer",
        out_shape=jax.ShapeDtypeStruct((ROWS, FEAT), BF16),
        in_specs=[pl.BlockSpec(memory_space=pltpu.HBM)] * 17,
        out_specs=pl.BlockSpec(memory_space=pltpu.VMEM),
        scratch_shapes=[
            bf(ROWS, CH), bf(ROWS, CH), f(TAPS, CH), f(CH), f(CH), f(CH), bf(CONV, FEAT), bf(ROWS, FEAT), f(FEAT),
            pltpu.VMEM((2, ROWS), jnp.int32), f(2, ROWS),
            bf(TP, 128, FEAT), bf(SIDE, SIDE, 128, FEAT), bf(128, D),
            bf(TP, 128, FEAT), bf(TP, 128, FEAT), bf(TP, 128, FEAT), bf(TP, 128, FEAT),
            pltpu.SemaphoreType.DMA((18,)),
            f(32 + ROWS, CH), f(ROWS, CH), bf(32, CH), bf(32, CH), f(8, ROWS), f(TP, 8, ROWS), bf(TP, ROWS, CH),
            bf(ROWS, FEAT), f(8, ROWS), f(TP, 8, ROWS), bf(TP, ROWS, FEAT),
            bf(SLOTS, ROWS), bf(ROWS, SLOTS), bf(ROWS, SLOTS),
            bf(SP, CAP, FEAT), bf(CHUNKS, SIDE, ROWS, FEAT), bf(CHUNKS, SIDE, ROWS, 128), bf(CHUNKS, SIDE, ROWS, 128),
            bf(CHUNKS + 1, TP, 128, 128), f(ROWS, FEAT), bf(CHUNKS, SP // CHUNKS, CAP, FEAT), bf(SP, CAP, FEAT),
            pltpu.SemaphoreType.DMA((SENDS,)), pltpu.SemaphoreType.DMA((RECVS,)),
        ],
        compiler_params=pltpu.CompilerParams(
            collective_id=0, has_side_effects=True, vmem_limit_bytes=60 * 2**20
        ),
    )(*args)


def solution(mesh):
    in_specs = (
        P("sp", "tp"), P("sp", "tp"), P(None, "tp"), P("tp"), P("tp"), P("tp"), P(None, "tp"), P("sp", "tp"), P("tp"),
        P("sp", None), P("sp", None), P("sp", None, "tp"), P("sp", None, "tp"), P("sp", None, "tp"),
        P(None, "tp"), P(None, "tp"), P(None, "tp"),
    )
    return jax.shard_map(shards, mesh=mesh, in_specs=in_specs, out_specs=P("sp", "tp"), check_vma=False)
```

```python
import heapq

import jax
import jax.numpy as jnp
from jax import lax
from jax.experimental import pallas as pl
from jax.experimental.pallas import tpu as pltpu
from jax.sharding import PartitionSpec as P

MESH = pl.DeviceIdType.MESH
F32 = jnp.float32
BF16 = jnp.bfloat16

SP, TP, SIDE = 32, 16, 4
ROWS, CH, FEAT = 256, 128, 256
CONV, D = 2048, 4096
TAPS = 31
CAP = 32
SLOTS = SP * CAP
CHUNKS = 4
HOPS = 4
SENDS, RECVS = 9 + 3 * CHUNKS, 6 + 24 * 2 + CHUNKS * (2 + 3 + 2 + 24)
ORDER = (3, 4, 2, 5, 1, 6, 0, 7)
EPS = 1e-6


def arrived(ref, sem):
    pltpu.make_async_copy(ref, ref, sem).wait()


class Copies:
    def __init__(self, send, recv):
        self.send, self.recv, self.sends, self.recvs, self.open = send, recv, 0, 0, []

    def group(self, ref):
        sem = self.send.at[self.sends]
        self.sends += 1
        self.open.append((ref, sem))
        return sem

    def landing(self):
        self.recvs += 1
        return self.recv.at[self.recvs - 1]

    def __call__(self, src, dst, target, send, recv):
        pltpu.make_async_remote_copy(
            src_ref=src, dst_ref=dst, send_sem=send, recv_sem=recv, device_id=target, device_id_type=MESH
        ).start()

    def drain(self):
        for ref, sem in self.open:
            arrived(ref, sem)


def wrap(i):
    return lax.rem(i + SIDE, SIDE)


class RingHalf:
    def __init__(self, copies, out, buf, lo, rows, first, y, x):
        self.copies, self.out, self.buf, self.lo, self.rows = copies, out, buf, lo, rows
        self.c1, self.c2 = (x, y) if first == "x" else (y, x)
        self.first = first

    def index(self, c1, c2):
        return c2 * SIDE + c1 if self.first == "x" else c1 * SIDE + c2

    def send(self, d1, d2, part, axis, step, sem=None):
        half = self.rows // 2
        lo, n = {0: (self.lo, self.rows), 1: (self.lo, half), 2: (self.lo + half, half)}[part]
        src = self.index(wrap(self.c1 + d1), wrap(self.c2 + d2))
        ref = self.buf.at[src, pl.ds(lo, n)]
        to = (
            self.index(wrap(self.c1 + step), self.c2)
            if axis == 1
            else self.index(self.c1, wrap(self.c2 + step))
        )
        sem = self.copies.landing() if sem is None else sem
        self.copies(ref, ref, {"tp": to}, self.out, sem)
        return sem

    def block(self, sem):
        arrived(self.buf.at[0, pl.ds(0, self.rows)], sem)

    def both(self, d):
        return self.send(d, 0, 0, 2, 1), self.send(d, 0, 0, 2, -1)

    def rounds(self):
        right = self.send(0, 0, 0, 1, 1)
        left = self.send(0, 0, 0, 1, -1)
        far = self.send(0, 0, 0, 1, 2)
        two = {0: self.both(0)}
        yield
        self.block(right)
        two[-1] = self.both(-1)
        self.block(left)
        two[1] = self.both(1)
        last = self.copies.landing()
        self.forward(two, 0, last)
        self.block(far)
        two[2] = self.both(2)
        yield
        self.forward(two, -1, last)
        self.forward(two, 1, last)
        self.forward(two, 2, last)
        yield
        arrived(self.buf.at[pl.ds(0, 2)], last)

    def lean(self):
        right = self.send(0, 0, 0, 1, 1)
        left = self.send(0, 0, 0, 1, -1)
        two = {0: self.both(0)}
        yield
        self.block(right)
        far = self.send(-1, 0, 1, 1, 1)
        two[-1] = self.both(-1)
        self.block(left)
        self.send(1, 0, 2, 1, -1, far)
        two[1] = self.both(1)
        last = self.copies.landing()
        self.forward(two, 0, last)
        yield
        self.block(far)
        two[2] = self.both(2)
        self.forward(two, -1, last)
        self.forward(two, 1, last)
        yield
        self.forward(two, 2, last)
        yield
        arrived(self.buf.at[pl.ds(0, 2)], last)

    def forward(self, two, d, last):
        right, left = two[d]
        self.block(right)
        self.send(d, -1, 1, 2, 1, last)
        self.block(left)
        self.send(d, 1, 2, 2, -1, last)


def gather_plane(copies, buf, rows, y, x, lean=False):
    out = copies.group(buf.at[pl.ds(0, TP - 1)])
    halves = (
        RingHalf(copies, out, buf, 0, rows // 2, "x", y, x),
        RingHalf(copies, out, buf, rows // 2, rows // 2, "y", y, x),
    )
    halves = [half.lean() if lean else half.rounds() for half in halves]
    for _ in range(HOPS + lean):
        for half in halves:
            next(half, None)
        yield


def run(steps):
    for _ in steps:
        pass


def ready(loads):
    while loads:
        arrived(*loads.pop())


def interleave(tasks):
    queue = [(at, n, task) for n, (at, task) in enumerate(tasks)]
    heapq.heapify(queue)
    while queue:
        now, n, task = heapq.heappop(queue)
        later = next(task, None)
        if later is not None:
            heapq.heappush(queue, (now + later, n, task))


def to_peers(copies, src, dst, me):
    out, sem = copies.group(dst.at[pl.ds(0, TP - 1)]), copies.landing()
    for k in range(1, TP):
        copies(src, dst.at[me], {"tp": lax.rem(me + k, TP)}, out, sem)
    return sem


def lanes(columns):
    rows = columns[0].shape[0]
    lane = lax.broadcasted_iota(jnp.int32, (rows, 128), 1)
    both = jnp.zeros((rows, 128), F32)
    for k, column in enumerate(columns):
        both = jnp.where(lane == k, column, both)
    return both.T


def columns(rows):
    n = rows[0].shape[1]
    sub = lax.broadcasted_iota(jnp.int32, (128, n), 0)
    both = jnp.zeros((128, n), F32)
    for k, row in enumerate(rows):
        both = jnp.where(sub == k, row, both)
    return both.T


def silu(v):
    return v / (1.0 + jnp.exp(-v))


def dot(a, b):
    return jnp.dot(a, b, preferred_element_type=F32)


def dot_t(a, b):
    return lax.dot_general(a, b, (((1,), (1,)), ((), ())), preferred_element_type=F32)


class Phases:
    def __init__(self):
        self.scope = None

    def __call__(self, name):
        if self.scope is not None:
            self.scope.__exit__(None, None, None)
        self.scope = jax.named_scope(name) if name else None
        if name:
            self.scope.__enter__()


def kernel(
    u_val, u_gate, conv_weight, conv_bias, ln_gain, ln_bias, proj, resid, norm_gain, ids, wts,
    e_gate, e_up, e_down, s_gate, s_up, s_down,
    out,
    v_val, v_gate, v_cw, v_cb, v_lg, v_lb, v_proj, v_resid, v_ng, v_ids, v_wts,
    ewt, w2, sgu, w_relay, w_lo, w_hi, s_lo, s_hi,
    in_sem,
    pad, conv, halo_out, halo_in, stat_out, stat_in, co, rm, ssq_out, ssq_in, na,
    disp, named_b, place_b, comb_hi, comb_lo, scale_row, scale_out, scale_in,
    sent, ya, rs_out, rs_relay, rs_mid, rs_in, hid, hid_last, back_out, back,
    send_sem, recv_sem,
):
    s, t = lax.axis_index("sp"), lax.axis_index("tp")
    y, x = t // SIDE, lax.rem(t, SIDE)

    phase = Phases()
    phase("start")
    barrier = pltpu.get_barrier_semaphore()
    for k in range(1, TP):
        pl.semaphore_signal(barrier, inc=1, device_id={"tp": lax.rem(t + k, TP)}, device_id_type=MESH)
    for k in range(1, SP):
        pl.semaphore_signal(barrier, inc=1, device_id={"sp": lax.rem(s + k, SP)}, device_id_type=MESH)

    loads = {}
    pairs = [
        (u_val, v_val), (u_gate, v_gate), (conv_weight, v_cw), (conv_bias, v_cb), (ln_gain, v_lg),
        (ln_bias, v_lb), (ids, v_ids), (wts, v_wts), (resid, v_resid), (norm_gain, v_ng), (proj, v_proj),
        (s_gate, sgu.at[pl.ds(0, 64)]), (s_up, sgu.at[pl.ds(64, 64)]),
    ]
    for k, (src, dst) in enumerate(pairs):
        copy = pltpu.make_async_copy(src, dst, in_sem.at[k])
        copy.start()
        loads[k] = copy
    for k in range(TP):
        for n, (src, dst, at) in enumerate(
            ((e_down.at[0], w_lo, 0), (e_down.at[0], w_hi, 64), (s_down, s_lo, 0), (s_down, s_hi, 64))
        ):
            pltpu.make_async_copy(
                src.at[pl.ds(64 * k, 64)], dst.at[k, pl.ds(at, 64)], in_sem.at[13 + n]
            ).start()
    downs = [(ref.at[pl.ds(0, TP // 2)], in_sem.at[13 + n]) for n, ref in enumerate((w_lo, w_hi, s_lo, s_hi))]
    for k in range(TP):
        for n, src in enumerate((e_gate, e_up)):
            pltpu.make_async_copy(
                src.at[0, :, pl.ds(FEAT * k, FEAT)], ewt.at[k, pl.ds(64 * n, 64)], in_sem.at[17]
            ).start()
    for k in range(TP):
        for ref, at in ((w_lo, 64), (w_hi, 0), (s_lo, 64), (s_hi, 0)):
            ref[k, pl.ds(at, 64), :] = jnp.zeros((64, FEAT), BF16)

    copies = Copies(send_sem, recv_sem)

    spread_out, spread_in, relay_in = copies.group(w2), copies.landing(), copies.landing()
    to_right, to_left = {"tp": y * SIDE + wrap(x + 1)}, {"tp": y * SIDE + wrap(x - 1)}
    sides = ((to_right, 1, (0, 1)), (to_left, -1, (2, 3)))

    def spread_far():
        for to, step, ks in sides:
            for k in ks:
                copies(ewt.at[SIDE * k + wrap(x + 2)], w_relay.at[k], to, spread_out, relay_in)

    def spread_near():
        phase("spread")
        for k in range(SIDE):
            for to, step, ks in sides:
                copies(ewt.at[SIDE * k + wrap(x + step)], w2.at[k, x], to, spread_out, spread_in)
        arrived(w_relay, relay_in)
        for to, step, ks in sides:
            for k in ks:
                copies(w_relay.at[k], w2.at[k, wrap(x - step)], to, spread_out, spread_in)
        yield None

    phase("gated")
    for k in (0, 1):
        loads[k].wait()
    gate = v_gate[...].astype(F32)
    gated = (v_val[...].astype(F32) / (1.0 + jnp.exp(-gate))).astype(BF16)
    pad[pl.ds(32, ROWS), :] = gated.astype(F32)
    halo_out[...] = gated[ROWS - 32 :]

    phase("slots")
    for k in (6, 7):
        loads[k].wait()
    id_rows = v_ids[...].astype(F32)
    id_row = jnp.concatenate([id_rows[0:1], id_rows[1:2]], axis=1)
    expert = lax.broadcasted_iota(jnp.int32, (SP, 2 * ROWS), 0).astype(F32)
    named = (expert == id_row).astype(F32)
    earlier = (
        lax.broadcasted_iota(jnp.int32, (2 * ROWS, 2 * ROWS), 0)
        < lax.broadcasted_iota(jnp.int32, (2 * ROWS, 2 * ROWS), 1)
    ).astype(F32).astype(BF16)
    place = jnp.sum(dot(named.astype(BF16), earlier) * named, axis=0, keepdims=True)
    slot = id_row * CAP + place
    named_b[...] = named.astype(BF16)
    slot_in = lax.broadcasted_iota(jnp.int32, (128, 2 * ROWS), 0).astype(F32)
    place_b[...] = jnp.where(slot_in == place, 1.0, 0.0).astype(BF16)
    slot_0, slot_1 = slot[:, :ROWS], slot[:, ROWS:]
    row = lax.broadcasted_iota(jnp.int32, (SLOTS, ROWS), 0).astype(F32)
    disp[...] = jnp.where((row == slot_0) | (row == slot_1), 1.0, 0.0).astype(BF16)
    cols = columns([slot_0, slot_1, v_wts[0:1, :], v_wts[1:2, :]])
    col = lax.broadcasted_iota(jnp.int32, (ROWS, SLOTS), 1).astype(F32)
    weight = jnp.where(col == cols[:, 0:1], cols[:, 2:3], 0.0) + jnp.where(
        col == cols[:, 1:2], cols[:, 3:4], 0.0
    )
    high = weight.astype(BF16)
    comb_hi[...] = high
    comb_lo[...] = (weight - high.astype(F32)).astype(BF16)

    phase("barrier")
    pl.semaphore_wait(barrier, TP - 1 + SP - 1)

    phase("halo")
    halo = copies.landing()
    copies(halo_out, halo_in, {"sp": lax.rem(s + 1, SP)}, copies.group(halo_in), halo)
    arrived(ewt, in_sem.at[17])
    spread_far()
    for k in range(SIDE):
        w2[k, x] = ewt[SIDE * k + x]
    for k in (2, 3, 4, 5):
        loads[k].wait()
    arrived(halo_in, halo)
    pad[pl.ds(0, 32), :] = jnp.where(s == 0, 0.0, halo_in[...].astype(F32))
    phase("conv")
    for part in range(2):
        total = jnp.broadcast_to(v_cb[...].reshape(1, CH), (128, CH))
        for tap in range(TAPS):
            total = total + v_cw[tap : tap + 1, :] * pad[pl.ds(128 * part + 2 + tap, 128), :]
        conv[pl.ds(128 * part, 128), :] = total

    phase("stats")
    mine = conv[...]
    mean = jnp.sum(mine, axis=1, keepdims=True) * (1.0 / CH)
    off = mine - mean
    stat_out[...] = lanes([mean, jnp.sum(off * off, axis=1, keepdims=True)])[0:8]
    stat_out[2:3, 0:CH] = v_lg[...].reshape(1, CH)
    stat_out[3:4, 0:CH] = v_lb[...].reshape(1, CH)
    stats = to_peers(copies, stat_out, stat_in, t)
    co[t] = off.astype(BF16)
    gather = gather_plane(copies, co, ROWS, y, x)
    next(gather)
    stat_in[t] = stat_out[...]
    phase("gather_co0")
    next(gather)
    phase("stats_wait")
    arrived(stat_in.at[pl.ds(0, TP - 1)], stats)
    means = stat_in[:, 0, :]
    total_mean = jnp.sum(means, axis=0, keepdims=True) * (1.0 / TP)
    off = means - total_mean
    var = (
        jnp.sum(stat_in[:, 1, :], axis=0, keepdims=True) + CH * jnp.sum(off * off, axis=0, keepdims=True)
    ) * (1.0 / CONV)
    around = [(dy, dx) for dy in (0, 1, 3) for dx in (0, 1, 3)]
    around += [(2, dx) for dx in range(SIDE)] + [(dy, 2) for dy in (0, 1, 3)]
    around = [wrap(y + dy) * SIDE + wrap(x + dx) for dy, dx in around]
    cols = columns([stat_in[k, 0:1, :] - total_mean for k in around] + [lax.rsqrt(var + EPS)])
    rstd = jnp.broadcast_to(cols[:, TP : TP + 1], (ROWS, CH))

    def normed(n):
        k = around[n]
        v = (co[k].astype(F32) + cols[:, n : n + 1]) * rstd
        return silu(v * stat_in[k, 2:3, 0:CH] + stat_in[k, 3:4, 0:CH]).astype(BF16)

    def projected(n):
        w = [v_proj[pl.ds(pl.multiple_of(CH * around[m], CH), CH), :] for m in (n, n + 1)]
        return dot(jnp.concatenate([normed(n), normed(n + 1)], axis=1), jnp.concatenate(w, axis=0))

    phase("gather_co1")
    next(gather)
    phase("project")
    for k in (8, 9, 10):
        loads[k].wait()
    acc = v_resid[...].astype(F32)
    for n in range(0, 8, 2):
        acc = acc + projected(n)
    phase("gather_co2")
    next(gather)
    phase("project_end")
    for n in range(8, TP, 2):
        acc = acc + projected(n)
    mid = acc.astype(BF16)
    rm[...] = mid
    wide = mid.astype(F32)
    ssq_out[...] = lanes([jnp.sum(wide * wide, axis=1, keepdims=True)])[0:8]
    squares = to_peers(copies, ssq_out, ssq_in, t)
    ssq_in[t] = ssq_out[...]
    na[t] = (wide * v_ng[...].reshape(1, FEAT)).astype(BF16)
    phase("dispatch")
    rows = dot(disp[...], na[t]).astype(BF16)
    sent[...] = rows.reshape(SP, CAP, FEAT)
    moves_out = copies.group(sent.at[pl.ds(0, SP - 1)])
    moves = [copies.landing() for c in range(CHUNKS)]

    def dispatch(c):
        phase(f"send{c}")
        for j in ORDER:
            k = CHUNKS * j + c
            if k:
                e = lax.rem(s + SP - k, SP)
                copies(sent.at[e], ya.at[c, y, pl.ds(CAP * j, CAP)], {"sp": e}, moves_out, moves[c])
        yield None

    scales_out = copies.group(scale_out.at[pl.ds(0, SP - 1)])
    scales = [copies.landing() for c in range(CHUNKS)]

    def rescale():
        phase("ssq")
        arrived(ssq_in.at[pl.ds(0, TP - 1)], squares)
        scale = lax.rsqrt(jnp.sum(ssq_in[:, 0, :], axis=0, keepdims=True) * (1.0 / D) + EPS)
        scale_row[...] = scale
        high = scale.astype(BF16)
        both = jnp.zeros((SP, 128), F32)
        for n in range(2):
            at = pl.ds(ROWS * n, ROWS)
            for part in (high, (scale - high.astype(F32)).astype(BF16)):
                both = both + dot_t(named_b[:, at] * part, place_b[:, at])
        scale_out[...] = both.reshape(SP, 1, 128)
        for c in range(CHUNKS):
            for j in ORDER:
                k = CHUNKS * j + c
                if k:
                    e = lax.rem(s + SP - k, SP)
                    copies(scale_out.at[e], scale_in.at[c, j], {"sp": e}, scales_out, scales[c])
        scale_in[0, 0] = scale_out[s]
        yield None

    ya[0, y, pl.ds(0, CAP), :] = sent[s]
    lane = lax.broadcasted_iota(jnp.int32, (128, 128), 1)

    def hidden(acc):
        h = silu(acc) * pltpu.roll(acc, 64, axis=1)
        return jnp.where(lane < 64, h[:128], pltpu.roll(h[128:], 64, axis=1)).astype(BF16)

    def down(buf, at, lo, hi):
        both = []
        for ref in (lo, hi):
            acc = jnp.zeros((128, FEAT), F32)
            for k in range(TP // 2):
                pair = jnp.concatenate([buf[2 * k, at, :], buf[2 * k + 1, at, :]], axis=1)
                acc = acc + dot(pair, ref[pl.ds(2 * k, 2)].reshape(2 * 128, FEAT))
            both.append(acc)
        return both

    def shared():
        steps = gather_plane(copies, na, ROWS, y, x, lean=True)
        for n in range(HOPS + 1):
            phase(f"na{n}")
            next(steps)
            yield 6.0 if n else 12.0
        phase("shared")
        for k in (11, 12):
            loads[k].wait()
        acc = jnp.zeros((ROWS, 128), F32)
        for k in range(TP):
            acc = acc + dot_t(na[k], sgu[:, pl.ds(FEAT * k, FEAT)])
        hid_last[t, pl.ds(128, 128), :] = hidden(acc * columns([scale_row[...]])[:, 0:1])

    own_rows = shared()
    returns_out, returns = copies.group(back.at[pl.ds(0, SP - 1)]), copies.landing()

    def routed(c):
        phase(f"arrive{c}")
        arrived(ya.at[c, 0, pl.ds(0 if c else CAP, ROWS if c else ROWS - CAP)], moves[c])
        out = copies.group(ya.at[c, pl.ds(0, 3)])
        a, b, far = copies.landing(), copies.landing(), copies.landing()
        up_y, down_y = {"tp": wrap(y + 1) * SIDE + x}, {"tp": wrap(y - 1) * SIDE + x}
        copies(ya.at[c, y], ya.at[c, y], up_y, out, a)
        copies(ya.at[c, y], ya.at[c, y], down_y, out, b)
        yield 4.8
        phase(f"ya{c}")
        arrived(ya.at[c, 0], a)
        at = ya.at[c, wrap(y - 1), pl.ds(0, 128)]
        copies(at, at, up_y, out, far)
        arrived(ya.at[c, 0], b)
        at = ya.at[c, wrap(y + 1), pl.ds(128, 128)]
        copies(at, at, down_y, out, far)
        yield 4.0
        phase(f"yb{c}")
        arrived(ya.at[c, 0], far)
        if c == 0:
            arrived(w2.at[pl.ds(0, 3)], spread_in)
        phase(f"up{c}")
        acc = jnp.zeros((ROWS, 4 * 128), F32)
        for k in range(SIDE):
            acc = acc + dot_t(ya[c, k], w2[k].reshape(4 * 128, FEAT))
        for k in range(SIDE):
            rs_out[c, k] = acc[:, 128 * k : 128 * (k + 1)].astype(BF16)
        out, relay, parts = copies.group(rs_out.at[c, pl.ds(0, 3)]), copies.landing(), copies.landing()
        right, left, lo, hi = wrap(x + 1), wrap(x - 1), pl.ds(0, 128), pl.ds(128, 128)
        to_r, to_l = {"tp": y * SIDE + right}, {"tp": y * SIDE + left}
        copies(rs_out.at[c, wrap(x + 2), lo], rs_relay.at[c, 0], to_r, out, relay)
        copies(rs_out.at[c, wrap(x + 2), hi], rs_relay.at[c, 1], to_l, out, relay)
        copies(rs_out.at[c, right, hi], rs_in.at[c, 0, hi], to_r, out, parts)
        copies(rs_out.at[c, left, lo], rs_in.at[c, 1, lo], to_l, out, parts)
        yield 3.5
        phase(f"relay{c}")
        arrived(rs_relay.at[c], relay)
        rs_mid[c, 0] = (rs_out[c, right, lo, :].astype(F32) + rs_relay[c, 0].astype(F32)).astype(BF16)
        rs_mid[c, 1] = (rs_out[c, left, hi, :].astype(F32) + rs_relay[c, 1].astype(F32)).astype(BF16)
        copies(rs_mid.at[c, 0], rs_in.at[c, 0, lo], to_r, out, parts)
        copies(rs_mid.at[c, 1], rs_in.at[c, 1, hi], to_l, out, parts)
        yield 3.0
        phase(f"rs{c}")
        arrived(rs_in.at[c], parts)
        acc = rs_out[c, x].astype(F32) + rs_in[c, 0].astype(F32) + rs_in[c, 1].astype(F32)
        first = 0 if c else 1
        arrived(scale_in.at[c, pl.ds(first, SP // CHUNKS - first)], scales[c])
        turned = jnp.concatenate(
            [scale_in[c].reshape(SP // CHUNKS, 128), jnp.zeros((128 - SP // CHUNKS, 128), F32)], axis=0
        ).T
        acc = acc * jnp.concatenate(
            [jnp.broadcast_to(turned[0:CAP, j : j + 1], (CAP, 128)) for j in range(SP // CHUNKS)], axis=0
        )
        if c < CHUNKS - 1:
            buf, rows = hid.at[c], 128
        else:
            run(own_rows)
            phase(f"hid{c}0")
            buf, rows = hid_last, 256
        buf[t, pl.ds(0, 128), :] = hidden(acc)
        steps = gather_plane(copies, buf, rows, y, x)
        next(steps)
        for n in range(1, HOPS):
            yield 3.2
            phase(f"hid{c}{n}")
            next(steps)
        ready(downs)
        phase(f"down{c}")
        lo, hi = down(buf, pl.ds(0, 128), w_lo, w_hi)
        back_out[c, pl.ds(0, 4)] = lo.astype(BF16).reshape(4, CAP, FEAT)
        back_out[c, pl.ds(4, 4)] = hi.astype(BF16).reshape(4, CAP, FEAT)
        for j in ORDER:
            k = CHUNKS * j + c
            if k:
                copies(back_out.at[c, j], back.at[s], {"sp": lax.rem(s + k, SP)}, returns_out, returns)

    tasks = [(0.0, dispatch(0)), (0.1, dispatch(1)), (0.2, spread_near()), (2.0, own_rows)]
    tasks += [(5.0, rescale()), (5.1, dispatch(2)), (5.2, dispatch(3))]
    tasks += [(at, routed(c)) for c, at in enumerate((8.0, 15.5, 20.0, 26.0))]
    interleave(tasks)
    back[s] = back_out[0, 0]
    phase("shared_down")
    own = rm[...].astype(F32) + jnp.concatenate(down(hid_last, pl.ds(128, 128), s_lo, s_hi), axis=0)
    phase("back_wait")
    arrived(back.at[pl.ds(0, SP - 1)], returns)
    phase("combine")
    full = back[...].reshape(SLOTS, FEAT)
    acc = own + dot(comb_hi[...], full) + dot(comb_lo[...], full)
    out[...] = acc.astype(BF16)
    phase("drain")
    copies.drain()
    assert (copies.sends, copies.recvs) == (SENDS, RECVS), (copies.sends, copies.recvs)
    phase(None)


def shards(*args):
    args = list(args)
    for k in (9, 10, 14, 15):
        args[k] = args[k].T
    for k in (11, 12):
        args[k] = jnp.swapaxes(args[k], 1, 2)
    bf, f = (lambda *shape: pltpu.VMEM(shape, BF16)), (lambda *shape: pltpu.VMEM(shape, F32))
    return pl.pallas_call(
        kernel,
        name="layer",
        out_shape=jax.ShapeDtypeStruct((ROWS, FEAT), BF16),
        in_specs=[pl.BlockSpec(memory_space=pltpu.HBM)] * 17,
        out_specs=pl.BlockSpec(memory_space=pltpu.VMEM),
        scratch_shapes=[
            bf(ROWS, CH), bf(ROWS, CH), f(TAPS, CH), f(CH), f(CH), f(CH), bf(CONV, FEAT), bf(ROWS, FEAT), f(FEAT),
            pltpu.VMEM((2, ROWS), jnp.int32), f(2, ROWS),
            bf(TP, 128, FEAT), bf(SIDE, SIDE, 128, FEAT), bf(128, D), bf(SIDE, 128, FEAT),
            bf(TP, 128, FEAT), bf(TP, 128, FEAT), bf(TP, 128, FEAT), bf(TP, 128, FEAT),
            pltpu.SemaphoreType.DMA((18,)),
            f(32 + ROWS, CH), f(ROWS, CH), bf(32, CH), bf(32, CH), f(8, ROWS), f(TP, 8, ROWS), bf(TP, ROWS, CH),
            bf(ROWS, FEAT), f(8, ROWS), f(TP, 8, ROWS), bf(TP, ROWS, FEAT),
            bf(SLOTS, ROWS), bf(SP, 2 * ROWS), bf(128, 2 * ROWS), bf(ROWS, SLOTS), bf(ROWS, SLOTS),
            f(1, ROWS), f(SP, 1, 128), f(CHUNKS, SP // CHUNKS, 1, 128),
            bf(SP, CAP, FEAT), bf(CHUNKS, SIDE, ROWS, FEAT), bf(CHUNKS, SIDE, ROWS, 128),
            bf(CHUNKS, 2, 128, 128), bf(CHUNKS, 2, 128, 128), bf(CHUNKS, 2, ROWS, 128),
            bf(CHUNKS - 1, TP, 128, 128), bf(TP, 256, 128), bf(CHUNKS, SP // CHUNKS, CAP, FEAT), bf(SP, CAP, FEAT),
            pltpu.SemaphoreType.DMA((SENDS,)), pltpu.SemaphoreType.DMA((RECVS,)),
        ],
        compiler_params=pltpu.CompilerParams(
            collective_id=0, has_side_effects=True, vmem_limit_bytes=60 * 2**20
        ),
    )(*args)


def solution(mesh):
    in_specs = (
        P("sp", "tp"), P("sp", "tp"), P(None, "tp"), P("tp"), P("tp"), P("tp"), P(None, "tp"), P("sp", "tp"), P("tp"),
        P("sp", None), P("sp", None), P("sp", None, "tp"), P("sp", None, "tp"), P("sp", None, "tp"),
        P(None, "tp"), P(None, "tp"), P(None, "tp"),
    )
    return jax.shard_map(shards, mesh=mesh, in_specs=in_specs, out_specs=P("sp", "tp"), check_vma=False)
```
